128 devices in a mesh: sp: 32 (over z, y, core), tp: 4 (over x).
Axes of the slice: x: 4, y: 4, z: 4, core: 2. Of those that a mesh axis runs over, the one named last changes fastest.
Arguments:
- query_rows: bfloat16 [32768, 1024], P('sp', 'tp'), may hold values from -6 to 6
- key_rows: bfloat16 [32768, 1024], P('sp', 'tp'), may hold values from -6 to 6
- value_rows: bfloat16 [32768, 1024], P('sp', 'tp'), may hold values from -6 to 6
- input_gate: float32 [8, 32768], P('tp', 'sp'), may hold values from -4 to 255
- forget_gate: float32 [8, 32768], P('tp', 'sp'), may hold values from -3 to 20
- output_gate: bfloat16 [32768, 1024], P('sp', 'tp'), may hold values from -6 to 6
- documents: int32 [32768], P('sp'), may hold values from 0 to 7, never falling along the last dimension, each value on 1 to 6144 neighbouring positions
- residual: bfloat16 [32768, 2048], P(('sp', 'tp')), may hold values from -6 to 6
- out_weight: bfloat16 [1024, 2048], P('tp'), may hold values from -0.375 to 0.375
- norm_gain: bfloat16 [2048], replicated, may hold values from 0.099609375 to 1.8984375
- gate_weight: bfloat16 [2048, 5632], P('sp', 'tp'), may hold values from -0.125 to 0.125
- up_weight: bfloat16 [2048, 5632], P('sp', 'tp'), may hold values from -0.125 to 0.125
- down_weight: bfloat16 [5632, 2048], P('tp', 'sp'), may hold values from -0.15625 to 0.15625
Outputs:
- layer_out: bfloat16 [32768, 2048], P(('sp', 'tp'))
The draws below stay inside these ranges and needn't reach their ends.
Inputs may be any that keep to these rules, and one draw needn't show every extreme that they name: `documents`: document numbers never fall along the positions; each document covers 1 to 6144 positions and one covers exactly 6144.
All inputs are finite; a program needn't handle non-finite values.
Results may differ from the reference program's by a relative error of at most 0.013.
Values may be sent and summed in bfloat16 or wider, within the bound.
No kernel may reach another device: no remote copies, remote signals or barrier semaphores. Data moves between devices by JAX's collectives and lax.ppermute only.
A program may use at most 128 MiB of HBM per device.

```python
import math
import jax
import jax.numpy as jnp
import numpy as np
from jax import lax

D = 2048
MEMORY_HEADS = 8
HD = 128
FF = 5632
BLOCK = 128
TOK_DEV = 1024
MW = 1024
PACKED_TOKENS = 32768
DOCS = 8
DOC_MOST = 6144
N_TP = 4


def draw_forget_gate(key, part):
    head_draw = jax.random.uniform(jax.random.fold_in(key, 11), (MEMORY_HEADS,), jnp.float32)
    slow_heads = head_draw < 0.5
    base_rate = jnp.where(slow_heads, 0.25 / PACKED_TOKENS, 1.0 / 40.0)
    block_count = PACKED_TOKENS // TOK_DEV
    block_scale = jnp.exp(jax.random.uniform(jax.random.fold_in(key, 12), (MEMORY_HEADS, block_count), jnp.float32, 0.0, math.log(3.0)))
    block_scale = jnp.repeat(block_scale, TOK_DEV, axis=1)
    jitter = 1.0 + 0.5 * jax.random.uniform(jax.random.fold_in(key, 13), (MEMORY_HEADS, PACKED_TOKENS), jnp.float32, -1.0, 1.0)
    spike_probability = base_rate[:, None] * block_scale * jitter
    spike_position = jax.random.randint(jax.random.fold_in(key, 14), (3,), 0, PACKED_TOKENS)
    spike_length = jax.random.uniform(jax.random.fold_in(key, 15), (MEMORY_HEADS, 3), jnp.float32, 0.22, 0.7)
    target_positions = jnp.arange(PACKED_TOKENS)
    match_count = (target_positions[None, :] == spike_position[:, None]).astype(jnp.float32)
    spike_probability = spike_probability + jnp.dot(spike_length, match_count)
    return -jnp.log(jnp.expm1(spike_probability))


def draw_input_gate(key, part):
    base = jnp.clip(jax.random.normal(jax.random.fold_in(key, 21), (MEMORY_HEADS, PACKED_TOKENS), jnp.float32), -4.0, 4.0)
    return base


def block_levels(rng, extent, pieces, smallest, largest):
    level, own = 1.0, jax.random.fold_in(rng, 6)
    for axis_at, blocks in pieces:
        steps = jnp.exp(jax.random.uniform(jax.random.fold_in(own, axis_at), (blocks,), jnp.float32, smallest / len(pieces), largest / len(pieces)))
        level = level * jnp.repeat(steps, extent[axis_at] // blocks).reshape([-1 if axis == axis_at else 1 for axis in range(len(extent))])
    return level


def length_profile(amount, total, bound, lean):
    loads = [(1 << 20) // math.isqrt(rank ** lean) + 1 for rank in range(2, amount + 1)]
    surplus, counts = total - bound - (amount - 1), [1] * (amount - 1)
    while surplus > 0:
        movable = [i for i in range(amount - 1) if counts[i] < bound]
        mass, remaining = sum([loads[i] for i in movable]), surplus
        for i in movable:
            more = min(bound - counts[i], max(1, remaining * loads[i] // mass), surplus)
            counts[i] = counts[i] + more
            surplus = surplus - more
    return np.array([bound] + counts)


def uneven(rng, count, total, reach, slope):
    if count == 2:
        one = jax.random.randint(rng, (), max(1, total - reach), min(reach, total - 1) + 1)
        return jnp.stack([one, total - one])
    sizes = jnp.asarray(length_profile(count, total, reach, slope), jnp.int32)
    twos = (count - 1) // 2
    source_of, sink = sizes[1:1 + 2 * twos:2], sizes[2:2 + 2 * twos:2]
    slack = jnp.minimum(source_of - 1, reach - sink)
    shifted = jax.random.randint(jax.random.fold_in(rng, 1), (twos,), 0, 1 << 20) % (slack + 1)
    sizes = sizes.at[1:1 + 2 * twos:2].set(source_of - shifted).at[2:2 + 2 * twos:2].set(sink + shifted)
    return sizes[jax.random.permutation(jax.random.fold_in(rng, 2), count)]


def centred(key, extent, deviation, limit, shards=(), dtype=jnp.bfloat16):
    level = block_levels(key, extent, shards, -0.22, 0.18) if shards else 1.0
    result = jax.random.normal(key, extent, jnp.float32) * deviation * level
    return jnp.minimum(jnp.maximum(result, -limit), limit).astype(dtype)


def setup_inputs(seed: int = 0) -> dict:
    splits = jax.random.split(jax.random.key(seed), 14)
    query_rows = centred(splits[0], (PACKED_TOKENS, MW), 1.0, 6.0, ((0, 32), (1, 4)))
    key_rows = centred(splits[1], (PACKED_TOKENS, MW), 1.0, 6.0, ((0, 32), (1, 4)))
    value_rows = centred(splits[2], (PACKED_TOKENS, MW), 1.0, 6.0, ((0, 32), (1, 4)))
    input_gate = draw_input_gate(jax.random.fold_in(splits[13], 71), 0)
    forget_gate = draw_forget_gate(jax.random.fold_in(splits[13], 71), 0)
    output_gate = centred(splits[5], (PACKED_TOKENS, MW), 1.5, 6.0, ((0, 32), (1, 4)))
    documents = jnp.searchsorted(jnp.cumsum(uneven(splits[6], DOCS, PACKED_TOKENS, DOC_MOST, 1)), jnp.arange(PACKED_TOKENS), side="right").astype(jnp.int32)
    residual = centred(splits[7], (PACKED_TOKENS, D), 1.0, 6.0, ((0, 128),))
    out_weight = centred(splits[8], (MW, D), (MW // 4) ** -0.5, 0.375, ((0, 4),))
    norm_gain = jnp.clip(1.0 + 0.18 * jax.random.normal(splits[9], (D,), jnp.float32), 0.099609375, 1.8984375).astype(jnp.bfloat16)
    gate_weight = centred(splits[10], (D, FF), D ** -0.5, 0.125, ((0, 32), (1, 4)))
    up_weight = centred(splits[11], (D, FF), D ** -0.5, 0.125, ((0, 32), (1, 4)))
    down_weight = centred(splits[12], (FF, D), (FF // 4) ** -0.5, 0.15625, ((0, 4), (1, 32)))
    return dict(query_rows=query_rows, key_rows=key_rows, value_rows=value_rows, input_gate=input_gate, forget_gate=forget_gate, output_gate=output_gate, documents=documents, residual=residual, out_weight=out_weight, norm_gain=norm_gain, gate_weight=gate_weight, up_weight=up_weight, down_weight=down_weight)


neg_large = -1e+30
norm_eps = 1e-06
highest = lax.Precision.HIGHEST

def block_step(carried, inputs):
    memory, normer, stab_prev, carry_doc = carried
    queries, key_float, value_float, gate_in, log_forget, docs = inputs
    cumlog = jnp.cumsum(log_forget, axis=1)
    length = docs.shape[0]
    target_positions = jnp.arange(length)
    same_doc = (docs[:, None] == docs[None, :]) & (target_positions[:, None] >= target_positions[None, :])
    log_weight = jnp.where(same_doc[None], cumlog[:, :, None] - cumlog[:, None, :] + gate_in[:, None, :], neg_large)
    carried_log = jnp.where((docs == carry_doc)[None, :], cumlog + stab_prev[:, None], neg_large)
    stabilizer = jnp.maximum(carried_log, lax.optimization_barrier(jnp.max(log_weight, axis=2)))
    scores = jnp.einsum('lhd,shd->hls', queries, key_float, precision=highest)
    weighted = scores * jnp.exp(log_weight - stabilizer[:, :, None])
    carried_scale = jnp.exp(carried_log - stabilizer)
    numerator = carried_scale[:, :, None] * jnp.einsum('lhd,hde->hle', queries, memory, precision=highest)
    numerator = numerator + jnp.einsum('hls,she->hle', weighted, value_float, precision=highest)
    denominator = carried_scale * jnp.einsum('lhd,hd->hl', queries, normer, precision=highest) + lax.optimization_barrier(jnp.sum(weighted, axis=2))
    outputs = numerator / jnp.maximum(jnp.abs(denominator), 1.0)[:, :, None]
    last_doc = docs[-1]
    inject_log = jnp.where((docs == last_doc)[None, :], cumlog[:, -1:] - cumlog + gate_in, neg_large)
    inject_max = lax.optimization_barrier(jnp.max(inject_log, axis=1))
    weights = jnp.exp(inject_log - inject_max[:, None])
    continues = carry_doc == last_doc
    stab_new = jnp.where(continues, jnp.maximum(cumlog[:, -1] + stab_prev, inject_max), inject_max)
    decay_scale = jnp.where(continues, jnp.exp(cumlog[:, -1] + stab_prev - stab_new), 0.0)
    inject = jnp.exp(inject_max - stab_new)
    memory_step = jnp.einsum('lhd,lhe->hde', key_float * weights.T[:, :, None], value_float, precision=highest)
    normer_step = jnp.einsum('hl,lhd->hd', weights, key_float, precision=highest)
    memory = decay_scale[:, None, None] * memory + inject[:, None, None] * memory_step
    normer = decay_scale[:, None] * normer + inject[:, None] * normer_step
    return ((memory, normer, stab_new, last_doc), jnp.transpose(outputs, (1, 0, 2)))

def run_blocks(queries, key_float, value_float, gate_in, log_forget, docs, start_state):
    length, heads, width = queries.shape
    count = length // BLOCK
    inputs = (queries.reshape(count, BLOCK, heads, width), key_float.reshape(count, BLOCK, heads, width), value_float.reshape(count, BLOCK, heads, width), jnp.moveaxis(gate_in.reshape(heads, count, BLOCK), 1, 0), jnp.moveaxis(log_forget.reshape(heads, count, BLOCK), 1, 0), docs.reshape(count, BLOCK))
    final, outputs = lax.scan(block_step, start_state, inputs)
    return (outputs.reshape(length, heads, width), final)

def reference(query_rows, key_rows, value_rows, input_gate, forget_gate, output_gate, documents, residual, out_weight, norm_gain, gate_weight, up_weight, down_weight):
    queries = query_rows.astype(jnp.float32).reshape(PACKED_TOKENS, MEMORY_HEADS, HD) * HD ** (-0.5)
    key_float = key_rows.astype(jnp.float32).reshape(PACKED_TOKENS, MEMORY_HEADS, HD)
    value_float = value_rows.astype(jnp.float32).reshape(PACKED_TOKENS, MEMORY_HEADS, HD)
    log_forget = jax.nn.log_sigmoid(forget_gate)
    start_state = (jnp.zeros((MEMORY_HEADS, HD, HD), jnp.float32), jnp.zeros((MEMORY_HEADS, HD), jnp.float32), jnp.full((MEMORY_HEADS,), neg_large, jnp.float32), jnp.array(-1, jnp.int32))
    cells, final = run_blocks(queries, key_float, value_float, input_gate, log_forget, documents, start_state)
    gated = (cells.reshape(PACKED_TOKENS, MW) * jax.nn.sigmoid(output_gate.astype(jnp.float32))).astype(jnp.bfloat16)
    projected = jnp.dot(gated, out_weight, preferred_element_type=jnp.float32)
    stream = residual.astype(jnp.float32) + projected
    normed = stream * lax.rsqrt(lax.optimization_barrier(jnp.mean(stream * stream, axis=1, keepdims=True)) + norm_eps)
    normed = (normed * norm_gain.astype(jnp.float32)).astype(jnp.bfloat16)
    gate_act = jnp.dot(normed, gate_weight, preferred_element_type=jnp.float32)
    up_act = jnp.dot(normed, up_weight, preferred_element_type=jnp.float32)
    hidden = (jax.nn.silu(gate_act) * up_act).astype(jnp.bfloat16)
    group = FF // N_TP
    down = jnp.zeros((PACKED_TOKENS, D), jnp.float32)
    for index in range(N_TP):
        partial_sum = jnp.dot(hidden[:, index * group:(index + 1) * group], down_weight[index * group:(index + 1) * group], preferred_element_type=jnp.float32)
        down = down + partial_sum.astype(jnp.bfloat16).astype(jnp.float32)
    return (stream + 0.5 * down).astype(jnp.bfloat16)
```

```python
import functools

import jax
import jax.numpy as jnp
from jax import lax
from jax.experimental import pallas as pl
from jax.experimental.pallas import tpu as pltpu
from jax.sharding import Mesh
from jax.sharding import PartitionSpec as P

HD = 128
SP = ("sp_0", "sp_1", "sp_2")
SP_TP = ("sp_0", "sp_1", "sp_2", "tp")
TOK = 1024
ROWS = 256
REACH = 6
STATE_ROWS = 304

neg_large = -1e30
norm_eps = 1e-06
bf16 = jnp.bfloat16
f32 = jnp.float32


def dims(a, b):
    return (((a,), (b,)), ((), ()))


def dot(a, b, ca=1, cb=0):
    return lax.dot_general(a, b, dims(ca, cb), preferred_element_type=f32)


def state_kernel(k_ref, v_ref, ig_ref, fg_ref, doc_ref, st_ref, a_ref, t_ref, s_ref):
    fg = fg_ref[...]
    lf = jnp.minimum(fg, 0.0) - jnp.log1p(jnp.exp(-jnp.abs(fg)))
    lane = lax.broadcasted_iota(jnp.int32, (2, TOK), 1)
    cum = lf
    step = 1
    while step < TOK:
        cum = cum + jnp.where(lane >= step, pltpu.roll(cum, step, 1), 0.0)
        step *= 2
    a = ig_ref[...] - cum
    a_ref[...] = a
    total = cum[:, TOK - 1 : TOK]
    doc = doc_ref[...]
    last = doc[:, TOK - 1 : TOK]
    al = jnp.where(doc == last, a, neg_large)
    amax = jnp.max(al, axis=1, keepdims=True)
    w = jnp.exp(al - amax)
    t_ref[...] = jnp.zeros((8, TOK), f32)
    t_ref[0:2, :] = w
    wt = jnp.transpose(t_ref[...])
    s_ref[...] = jnp.zeros((16, HD), f32)
    stab = total + amax
    for h in range(2):
        cols = slice(h * HD, (h + 1) * HD)
        kw = k_ref[:, cols].astype(f32) * wt[:, h : h + 1]
        s_ref[h : h + 1, :] = jnp.sum(kw, axis=0, keepdims=True)
        hi = kw.astype(bf16)
        lo = (kw - hi.astype(f32)).astype(bf16)
        v = v_ref[:, cols]
        mem = dot(hi, v, 0, 0) + dot(lo, v, 0, 0)
        st_ref[h * HD : (h + 1) * HD, :] = mem.astype(bf16)
        s_ref[2 + h : 3 + h, :] = jnp.broadcast_to(stab[h : h + 1, :], (1, HD))
        s_ref[4 + h : 5 + h, :] = jnp.broadcast_to(total[h : h + 1, :], (1, HD))
    s_ref[6:7, :] = jnp.broadcast_to(last.astype(f32) + 1.0, (1, HD))
    s = s_ref[...]
    hi = s.astype(bf16)
    rest = s - hi.astype(f32)
    mid = rest.astype(bf16)
    lo = (rest - mid.astype(f32)).astype(bf16)
    st_ref[256:272, :] = hi
    st_ref[272:288, :] = mid
    st_ref[288:304, :] = lo


def state_call(k, v, ig, fg, doc):
    return pl.pallas_call(
        state_kernel,
        out_shape=(
            jax.ShapeDtypeStruct((STATE_ROWS, HD), bf16),
            jax.ShapeDtypeStruct((2, TOK), f32),
        ),
        scratch_shapes=[pltpu.VMEM((8, TOK), f32), pltpu.VMEM((16, HD), f32)],
        name="state",
    )(k, v, ig, fg, doc)


def local_kernel(q_ref, k_ref, v_ref, a_ref, doc_ref, num_ref, aux_ref, t_ref):
    t_ref[...] = jnp.zeros((8, TOK), f32)
    docf = doc_ref[...].astype(f32)
    t_ref[0:1, :] = docf
    cols_t = jnp.transpose(t_ref[...])
    step = 256
    row = lax.broadcasted_iota(jnp.int32, (step, step), 0)
    col = lax.broadcasted_iota(jnp.int32, (step, step), 1)
    causal = row >= col
    lane = lax.broadcasted_iota(jnp.int32, (step, HD), 1)
    for r in range(TOK // step):
        rows = slice(r * step, (r + 1) * step)
        drow = cols_t[rows, 0:1]
        aux = jnp.zeros((step, HD), f32)
        for h in range(2):
            cols = slice(h * HD, (h + 1) * HD)
            q = q_ref[rows, cols]
            logs, top = [], None
            for c in range(r + 1):
                at = slice(c * step, (c + 1) * step)
                ok = drow == docf[:, at]
                if c == r:
                    ok = ok & causal
                logit = jnp.where(ok, a_ref[h : h + 1, at], neg_large)
                best = jnp.max(logit, axis=1, keepdims=True)
                top = best if top is None else jnp.maximum(top, best)
                logs.append(logit)
            num = jnp.zeros((step, HD), f32)
            den = jnp.zeros((step, 1), f32)
            for c in range(r + 1):
                at = slice(c * step, (c + 1) * step)
                score = dot(q, k_ref[at, cols], 1, 1) * HD ** (-0.5)
                p = score * jnp.exp(logs[c] - top)
                den = den + jnp.sum(p, axis=1, keepdims=True)
                v = v_ref[at, cols]
                hi = p.astype(bf16)
                lo = (p - hi.astype(f32)).astype(bf16)
                num = num + dot(hi, v) + dot(lo, v)
            num_ref[rows, cols] = num
            aux = jnp.where(lane == h, top, aux)
            aux = jnp.where(lane == 2 + h, den, aux)
        aux = jnp.where(lane == 4, drow, aux)
        aux_ref[rows, :] = aux


def local_call(q, k, v, a, doc):
    return pl.pallas_call(
        local_kernel,
        out_shape=(
            jax.ShapeDtypeStruct((TOK, 2 * HD), f32),
            jax.ShapeDtypeStruct((TOK, HD), f32),
        ),
        scratch_shapes=[pltpu.VMEM((8, TOK), f32)],
        name="local",
    )(q, k, v, a, doc)


def join_kernel(*refs):
    states = refs[:REACH]
    q_ref, num_ref, aux_ref, og_ref, out_ref = refs[REACH:]
    small = [
        s[256:272, :].astype(f32) + s[272:288, :].astype(f32) + s[288:304, :].astype(f32)
        for s in states
    ]
    carry = small[0][6:7, :]
    totals = jnp.zeros((2, HD), f32)
    logs = []
    for d in range(REACH):
        mine = (small[d][6:7, :] == carry) & (carry > 0.5)
        logs.append(jnp.where(mine, small[d][2:4, :] + totals, neg_large))
        totals = totals + small[d][4:6, :]
    stab = functools.reduce(jnp.maximum, logs)
    scale = [jnp.where(l > 0.5 * neg_large, jnp.exp(l - stab), 0.0) for l in logs]
    aux = aux_ref[...]
    continues = aux[:, 4:5] + 1.0 == carry[:, 0:1]
    for h in range(2):
        cols = slice(h * HD, (h + 1) * HD)
        mem = jnp.zeros((HD, HD), f32)
        normer = jnp.zeros((1, HD), f32)
        for d in range(REACH):
            mem = mem + scale[d][h : h + 1, :] * states[d][cols, :].astype(f32)
            normer = normer + scale[d][h : h + 1, :] * small[d][h : h + 1, :]
        q = q_ref[:, cols]
        hi = mem.astype(bf16)
        lo = (mem - hi.astype(f32)).astype(bf16)
        carried = dot(q, hi) + dot(q, lo)
        qn = jnp.sum(q.astype(f32) * normer, axis=1, keepdims=True)
        m_loc = aux[:, h : h + 1]
        prev = jnp.where(continues, stab[h : h + 1, 0:1], neg_large)
        m = jnp.maximum(m_loc, prev)
        keep = jnp.exp(m_loc - m)
        back = jnp.where(continues, jnp.exp(prev - m), 0.0) * HD ** (-0.5)
        den = keep * aux[:, 2 + h : 3 + h] + back * qn
        num = keep * num_ref[:, cols] + back * carried
        cell = num / jnp.maximum(jnp.abs(den), 1.0)
        og = og_ref[:, cols].astype(f32)
        out_ref[:, cols] = (cell * jax.nn.sigmoid(og)).astype(bf16)


def join_call(states, q, num, aux, og):
    step = 256
    rows = lambda w: pl.BlockSpec((step, w), lambda i: (i, 0))
    whole = pl.BlockSpec((STATE_ROWS, HD), lambda i: (0, 0))
    return pl.pallas_call(
        join_kernel,
        grid=(TOK // step,),
        in_specs=[whole] * REACH + [rows(2 * HD), rows(2 * HD), rows(HD), rows(2 * HD)],
        out_specs=rows(2 * HD),
        out_shape=jax.ShapeDtypeStruct((TOK, 2 * HD), bf16),
        name="join",
    )(*states, q, num, aux, og)


def proj_kernel(at_ref, g0, g1, g2, g3, w0, w1, w2, w3, r0, r1, r2, r3, gain, n_ref, s_ref):
    p = pl.program_id(0)
    acc = dot(g0[...], w0[...]) + dot(g1[...], w1[...])
    acc = acc + dot(g2[...], w2[...]) + dot(g3[...], w3[...])

    def finish(res):
        stream = acc + res[...].astype(f32)
        mean = jnp.mean(stream * stream, axis=1, keepdims=True)
        normed = stream * lax.rsqrt(mean + norm_eps) * gain[...].astype(f32)
        n_ref[...] = normed.astype(bf16)
        return stream

    @pl.when(p == 0)
    def _():
        s_ref[...] = finish(r0)

    for k, r in ((1, r1), (2, r2), (3, r3)):

        @pl.when(p == k)
        def _(r=r):
            finish(r)


def proj_call(at, gated, weights, residuals, gain):
    d = residuals[0].shape[1]
    g_spec = pl.BlockSpec((ROWS, 2 * HD), lambda i, at: (at[i], 0))
    whole = pl.BlockSpec((ROWS, d), lambda i, at: (0, 0))
    return pl.pallas_call(
        proj_kernel,
        grid_spec=pltpu.PrefetchScalarGridSpec(
            num_scalar_prefetch=1,
            grid=(4,),
            in_specs=[g_spec] * 4 + [whole] * 8 + [pl.BlockSpec((1, d), lambda i, at: (0, 0))],
            out_specs=(
                pl.BlockSpec((ROWS, d), lambda i, at: (i, 0)),
                pl.BlockSpec((ROWS, d), lambda i, at: (0, 0)),
            ),
        ),
        out_shape=(
            jax.ShapeDtypeStruct((4 * ROWS, d), bf16),
            jax.ShapeDtypeStruct((ROWS, d), f32),
        ),
        name="proj",
    )(at, *gated, *weights, *residuals, gain)


def mixer_kernel(steps, n_ref, gu_ref, dn_ref, o_ref, h_ref):
    i = pl.program_id(0)

    @pl.when(i < steps)
    def _():
        both = dot(n_ref[...], gu_ref[...])
        gate, up = both[:, :HD], both[:, HD:]
        h_ref[i] = (gate * jax.nn.sigmoid(gate) * up).astype(bf16)

    @pl.when(i >= steps)
    def _():
        hidden = jnp.concatenate([h_ref[k] for k in range(steps)], axis=1)
        o_ref[...] = dot(hidden, dn_ref[...], 1, 1).astype(bf16)


def mixer_call(normed, gate_up, down_t, rows, block):
    d = normed.shape[1]
    units = down_t.shape[1]
    steps = units // HD
    wide = 512
    outs = d // wide
    return pl.pallas_call(
        functools.partial(mixer_kernel, steps),
        grid=(steps + outs,),
        in_specs=[
            pl.BlockSpec((rows, d), lambda i: (block, 0)),
            pl.BlockSpec((d, 2 * HD), lambda i: (0, jnp.minimum(i, steps - 1))),
            pl.BlockSpec((wide, units), lambda i: (jnp.maximum(i - steps, 0), 0)),
        ],
        out_specs=pl.BlockSpec((rows, wide), lambda i: (0, jnp.maximum(i - steps, 0))),
        out_shape=jax.ShapeDtypeStruct((rows, d), bf16),
        scratch_shapes=[pltpu.VMEM((steps, rows, HD), bf16)],
        name="mixer",
    )(normed, gate_up, down_t)


def shift(x, by, axis="tp", n=4):
    return lax.ppermute(x, axis, [(i, (i + by) % n) for i in range(n)])


def relative(x):
    return (x, shift(x, 1), shift(x, -1), shift(x, 2))


def body(
    query_rows,
    key_rows,
    value_rows,
    input_gate,
    forget_gate,
    output_gate,
    documents,
    residual,
    out_weight,
    norm_gain,
    gate_weight,
    up_weight,
    down_weight,
):
    me = lax.axis_index("tp")
    core = lax.axis_index("sp_2")
    docs = documents.reshape(1, TOK)
    k_rows, units = gate_weight.shape
    tiles = units // HD
    pair = jnp.concatenate(
        [gate_weight.reshape(k_rows, tiles, 1, HD), up_weight.reshape(k_rows, tiles, 1, HD)], axis=2
    ).reshape(k_rows, 2 * units)
    gate_up = lax.all_gather(pair, SP, axis=0, tiled=True)
    down_t = lax.all_gather(down_weight.T, SP, axis=0, tiled=True)
    state, a = state_call(key_rows, value_rows, input_gate, forget_gate, docs)
    states = [
        lax.ppermute(state, SP, [(i, i + d) for i in range(32 - d)]) for d in range(1, REACH + 1)
    ]
    residuals = relative(residual)
    half = lax.dynamic_slice_in_dim(out_weight, core * (ROWS // 2), ROWS // 2, 0)
    halves = [shift(half, by) for by in (1, -1, 2)]
    weights = [out_weight]
    for mine in halves:
        other = shift(mine, 1, "sp_2", 2)
        weights.append(
            jnp.concatenate(
                [jnp.where(core == 0, mine, other), jnp.where(core == 0, other, mine)], axis=0
            )
        )
    num, aux = local_call(query_rows, key_rows, value_rows, a, docs)
    gated = join_call(states, query_rows, num, aux, output_gate)
    at = (me + jnp.array([0, 3, 1, 2], jnp.int32)) % 4
    normed, stream = proj_call(
        at, relative(gated), weights, residuals, norm_gain.reshape(1, -1)
    )
    own, left, right, opp = (slice(k * ROWS, (k + 1) * ROWS) for k in range(4))
    second = mixer_call(normed, gate_up, down_t, 2 * ROWS, 1)
    sent_right = shift(second[:ROWS], 1)
    sent_opp = shift(second[ROWS:], 2)
    first = mixer_call(normed, gate_up, down_t, 2 * ROWS, 0)
    sent_left = shift(first[ROWS:], -1)
    down = first[:ROWS].astype(f32) + sent_right.astype(f32)
    down = down + sent_left.astype(f32) + sent_opp.astype(f32)
    return (stream + 0.5 * down).astype(bf16)


def solution(mesh):
    torus = Mesh(mesh.devices.reshape(4, 4, 2, mesh.shape["tp"]), ("sp_0", "sp_1", "sp_2", "tp"))
    in_specs = (
        P(SP, "tp"),
        P(SP, "tp"),
        P(SP, "tp"),
        P("tp", SP),
        P("tp", SP),
        P(SP, "tp"),
        P(SP),
        P(SP_TP, None),
        P("tp", None),
        P(),
        P(SP, "tp"),
        P(SP, "tp"),
        P("tp", SP),
    )
    out_specs = P(SP_TP, None)
    return jax.shard_map(body, mesh=torus, in_specs=in_specs, out_specs=out_specs, check_vma=False)
```

```python
import functools

import jax
import jax.numpy as jnp
from jax import lax
from jax.experimental import pallas as pl
from jax.experimental.pallas import tpu as pltpu
from jax.sharding import Mesh
from jax.sharding import PartitionSpec as P

HD = 128
SP = ("sp_0", "sp_1", "sp_2")
SP_TP = ("sp_0", "sp_1", "sp_2", "tp")
TOK = 1024
ROWS = 256
STATE_ROWS = 304

neg_large = -1e30
norm_eps = 1e-06
bf16 = jnp.bfloat16
f32 = jnp.float32


def cost(us):
    return pl.CostEstimate(flops=int(us * 1e9), transcendentals=0, bytes_accessed=0)


def dims(a, b):
    return (((a,), (b,)), ((), ()))


def dot(a, b, ca=1, cb=0):
    return lax.dot_general(a, b, dims(ca, cb), preferred_element_type=f32)


def state_kernel(k_ref, v_ref, ig_ref, fg_ref, doc_ref, st_ref, a_ref, t_ref, s_ref):
    fg = fg_ref[...]
    lf = jnp.minimum(fg, 0.0) - jnp.log1p(jnp.exp(-jnp.abs(fg)))
    lane = lax.broadcasted_iota(jnp.int32, (2, TOK), 1)
    cum = lf
    step = 1
    while step < TOK:
        cum = cum + jnp.where(lane >= step, pltpu.roll(cum, step, 1), 0.0)
        step *= 2
    a = ig_ref[...] - cum
    a_ref[...] = a
    total = cum[:, TOK - 1 : TOK]
    doc = doc_ref[...]
    last = doc[:, TOK - 1 : TOK]
    al = jnp.where(doc == last, a, neg_large)
    amax = jnp.max(al, axis=1, keepdims=True)
    w = jnp.exp(al - amax)
    t_ref[...] = jnp.zeros((8, TOK), f32)
    t_ref[0:2, :] = w
    wt = jnp.transpose(t_ref[...])
    s_ref[...] = jnp.zeros((16, HD), f32)
    stab = total + amax
    for h in range(2):
        cols = slice(h * HD, (h + 1) * HD)
        kw = k_ref[:, cols].astype(f32) * wt[:, h : h + 1]
        s_ref[h : h + 1, :] = jnp.sum(kw, axis=0, keepdims=True)
        hi = kw.astype(bf16)
        lo = (kw - hi.astype(f32)).astype(bf16)
        v = v_ref[:, cols]
        mem = dot(hi, v, 0, 0) + dot(lo, v, 0, 0)
        st_ref[h * HD : (h + 1) * HD, :] = mem.astype(bf16)
        s_ref[2 + h : 3 + h, :] = jnp.broadcast_to(stab[h : h + 1, :], (1, HD))
        s_ref[4 + h : 5 + h, :] = jnp.broadcast_to(total[h : h + 1, :], (1, HD))
    s_ref[6:7, :] = jnp.broadcast_to(last.astype(f32) + 1.0, (1, HD))
    s = s_ref[...]
    hi = s.astype(bf16)
    rest = s - hi.astype(f32)
    mid = rest.astype(bf16)
    lo = (rest - mid.astype(f32)).astype(bf16)
    st_ref[256:272, :] = hi
    st_ref[272:288, :] = mid
    st_ref[288:304, :] = lo


def state_call(k, v, ig, fg, doc):
    return pl.pallas_call(
        state_kernel,
        out_shape=(
            jax.ShapeDtypeStruct((STATE_ROWS, HD), bf16),
            jax.ShapeDtypeStruct((2, TOK), f32),
        ),
        scratch_shapes=[pltpu.VMEM((8, TOK), f32), pltpu.VMEM((16, HD), f32)],
        cost_estimate=cost(4),
        name="state",
    )(k, v, ig, fg, doc)


def local_kernel(q_ref, k_ref, v_ref, a_ref, doc_ref, num_ref, aux_ref, t_ref):
    t_ref[...] = jnp.zeros((8, TOK), f32)
    docf = doc_ref[...].astype(f32)
    t_ref[0:1, :] = docf
    cols_t = jnp.transpose(t_ref[...])
    step = 256
    row = lax.broadcasted_iota(jnp.int32, (step, step), 0)
    col = lax.broadcasted_iota(jnp.int32, (step, step), 1)
    causal = row >= col
    lane = lax.broadcasted_iota(jnp.int32, (step, HD), 1)
    for r in range(TOK // step):
        rows = slice(r * step, (r + 1) * step)
        drow = cols_t[rows, 0:1]
        aux = jnp.zeros((step, HD), f32)
        for h in range(2):
            cols = slice(h * HD, (h + 1) * HD)
            q = q_ref[rows, cols]
            logs, top = [], None
            for c in range(r + 1):
                at = slice(c * step, (c + 1) * step)
                ok = drow == docf[:, at]
                if c == r:
                    ok = ok & causal
                logit = jnp.where(ok, a_ref[h : h + 1, at], neg_large)
                best = jnp.max(logit, axis=1, keepdims=True)
                top = best if top is None else jnp.maximum(top, best)
                logs.append(logit)
            num = jnp.zeros((step, HD), f32)
            den = jnp.zeros((step, 1), f32)
            for c in range(r + 1):
                at = slice(c * step, (c + 1) * step)
                score = dot(q, k_ref[at, cols], 1, 1) * HD ** (-0.5)
                p = score * jnp.exp(logs[c] - top)
                den = den + jnp.sum(p, axis=1, keepdims=True)
                v = v_ref[at, cols]
                hi = p.astype(bf16)
                lo = (p - hi.astype(f32)).astype(bf16)
                num = num + dot(hi, v) + dot(lo, v)
            num_ref[rows, cols] = num
            aux = jnp.where(lane == h, top, aux)
            aux = jnp.where(lane == 2 + h, den, aux)
        aux = jnp.where(lane == 4, drow, aux)
        aux_ref[rows, :] = aux


def local_call(q, k, v, a, doc):
    return pl.pallas_call(
        local_kernel,
        out_shape=(
            jax.ShapeDtypeStruct((TOK, 2 * HD), f32),
            jax.ShapeDtypeStruct((TOK, HD), f32),
        ),
        scratch_shapes=[pltpu.VMEM((8, TOK), f32)],
        cost_estimate=cost(7),
        name="local",
    )(q, k, v, a, doc)


def join_kernel(core_ref, far_ref, near_ref, q_ref, num_ref, aux_ref, og_ref, out_ref):
    is_second = (jnp.zeros((1, HD), jnp.int32) + core_ref[0]) == 1

    def small(ref, d):
        at = d * STATE_ROWS
        return (
            ref[at + 256 : at + 272, :].astype(f32)
            + ref[at + 272 : at + 288, :].astype(f32)
            + ref[at + 288 : at + 304, :].astype(f32)
        )

    far = [small(far_ref, d) for d in range(4)]
    near = [small(near_ref, d) for d in range(4)]
    carry = jnp.where(is_second, near[0][6:7, :], near[1][6:7, :])
    base = jnp.where(is_second, near[0][4:6, :], 0.0)
    entries = [(near_ref, 0, near[0], jnp.where(is_second, near[0][2:4, :], neg_large))]
    for d in range(1, 4):
        for ref, own, partner, later in (
            (far_ref, far[d], near[d], ~is_second),
            (near_ref, near[d], far[d], is_second),
        ):
            log = own[2:4, :] + base + jnp.where(later, partner[4:6, :], 0.0)
            mine = (own[6:7, :] == carry) & (carry > 0.5)
            entries.append((ref, d, own, jnp.where(mine, log, neg_large)))
        base = base + far[d][4:6, :] + near[d][4:6, :]
    stab = functools.reduce(jnp.maximum, [e[3] for e in entries])
    scale = [jnp.where(e[3] > 0.5 * neg_large, jnp.exp(e[3] - stab), 0.0) for e in entries]
    aux = aux_ref[...]
    continues = aux[:, 4:5] + 1.0 == carry[:, 0:1]
    for h in range(2):
        cols = slice(h * HD, (h + 1) * HD)
        mem = jnp.zeros((HD, HD), f32)
        normer = jnp.zeros((1, HD), f32)
        for (ref, d, own, _), s in zip(entries, scale):
            at = d * STATE_ROWS + h * HD
            mem = mem + s[h : h + 1, :] * ref[at : at + HD, :].astype(f32)
            normer = normer + s[h : h + 1, :] * own[h : h + 1, :]
        q = q_ref[:, cols]
        hi = mem.astype(bf16)
        lo = (mem - hi.astype(f32)).astype(bf16)
        carried = dot(q, hi) + dot(q, lo)
        qn = jnp.sum(q.astype(f32) * normer, axis=1, keepdims=True)
        m_loc = aux[:, h : h + 1]
        prev = jnp.where(continues, stab[h : h + 1, 0:1], neg_large)
        m = jnp.maximum(m_loc, prev)
        keep = jnp.exp(m_loc - m)
        back = jnp.where(continues, jnp.exp(prev - m), 0.0) * HD ** (-0.5)
        den = keep * aux[:, 2 + h : 3 + h] + back * qn
        num = keep * num_ref[:, cols] + back * carried
        cell = num / jnp.maximum(jnp.abs(den), 1.0)
        og = og_ref[:, cols].astype(f32)
        out_ref[:, cols] = (cell * jax.nn.sigmoid(og)).astype(bf16)


def join_call(core, far, near, q, num, aux, og):
    step = 256
    rows = lambda w: pl.BlockSpec((step, w), lambda i, core: (i, 0))
    whole = pl.BlockSpec((4 * STATE_ROWS, HD), lambda i, core: (0, 0))
    return pl.pallas_call(
        join_kernel,
        grid_spec=pltpu.PrefetchScalarGridSpec(
            num_scalar_prefetch=1,
            grid=(TOK // step,),
            in_specs=[whole] * 2 + [rows(2 * HD), rows(2 * HD), rows(HD), rows(2 * HD)],
            out_specs=rows(2 * HD),
        ),
        out_shape=jax.ShapeDtypeStruct((TOK, 2 * HD), bf16),
        cost_estimate=cost(6),
        name="join",
    )(core, far, near, q, num, aux, og)


BLOCKS = ((3, 0), (2, 1), (3, 1), (1, 0), (2, 0), (1, 1), (0, 0), (0, 1))
PART = 128


def proj_kernel(
    at_ref, core_ref, g0, g1, g2, g3, gain, own_w, own_r, left, right, opp_a, opp_b,
    p_left, p_right, p_opp_a, p_opp_b, n_ref, s_ref, w_v, r_v, w_sem, r_sem,
):
    i = pl.program_id(0)
    half = PART // 2
    mine = core_ref[0] * PART
    other = PART - mine
    to = lambda row, n: w_v.at[pl.ds(row, n), :]
    w_copies = [
        (own_w, to(0, ROWS)),
        (left.at[pl.ds(PART, PART), :], to(ROWS + mine, PART)),
        (p_left, to(ROWS + other, PART)),
        (right.at[pl.ds(PART, PART), :], to(2 * ROWS + mine, PART)),
        (p_right, to(2 * ROWS + other, PART)),
        (opp_a.at[pl.ds(PART, half), :], to(3 * ROWS + mine, half)),
        (opp_b.at[pl.ds(0, half), :], to(3 * ROWS + mine + half, half)),
        (p_opp_a, to(3 * ROWS + other, half)),
        (p_opp_b, to(3 * ROWS + other + half, half)),
    ]
    w_copies = [pltpu.make_async_copy(s, d, w_sem.at[k]) for k, (s, d) in enumerate(w_copies)]
    sources = [
        opp_a.at[pl.ds(0, PART), :],
        right.at[pl.ds(2 * PART, PART), :],
        opp_b.at[pl.ds(half, PART), :],
        left.at[pl.ds(0, PART), :],
        right.at[pl.ds(0, PART), :],
        left.at[pl.ds(2 * PART, PART), :],
        own_r.at[pl.ds(0, PART), :],
        own_r.at[pl.ds(PART, PART), :],
    ]
    r_copies = [pltpu.make_async_copy(s, r_v.at[k], r_sem.at[k]) for k, s in enumerate(sources)]

    @pl.when(i == 0)
    def _():
        for c in w_copies:
            c.start()
        for c in r_copies:
            c.start()
        for c in w_copies:
            c.wait()

    acc = dot(g0[...], w_v[0:ROWS, :]) + dot(g1[...], w_v[ROWS : 2 * ROWS, :])
    acc = acc + dot(g2[...], w_v[2 * ROWS : 3 * ROWS, :])
    acc = acc + dot(g3[...], w_v[3 * ROWS : 4 * ROWS, :])
    for k, c in enumerate(r_copies):

        @pl.when(i == k)
        def _(c=c):
            c.wait()

    stream = acc + r_v[i].astype(f32)
    mean = jnp.mean(stream * stream, axis=1, keepdims=True)
    normed = stream * lax.rsqrt(mean + norm_eps) * gain[...].astype(f32)
    n_ref[...] = normed.astype(bf16)
    s_ref[...] = stream


def proj_call(at, core, gated, gain, rest):
    d = gain.shape[1]
    g_spec = pl.BlockSpec((PART, 2 * HD), lambda i, at, core: (at[i], 0))
    anywhere = pl.BlockSpec(memory_space=pl.ANY)
    count = len(BLOCKS)
    return pl.pallas_call(
        proj_kernel,
        grid_spec=pltpu.PrefetchScalarGridSpec(
            num_scalar_prefetch=2,
            grid=(count,),
            in_specs=[g_spec] * 4
            + [pl.BlockSpec((1, d), lambda i, at, core: (0, 0))]
            + [anywhere] * len(rest),
            out_specs=(
                pl.BlockSpec((PART, d), lambda i, at, core: (i, 0)),
                pl.BlockSpec((PART, d), lambda i, at, core: (jnp.maximum(i - 6, 0), 0)),
            ),
            scratch_shapes=[
                pltpu.VMEM((4 * ROWS, d), bf16),
                pltpu.VMEM((count, PART, d), bf16),
                pltpu.SemaphoreType.DMA((9,)),
                pltpu.SemaphoreType.DMA((count,)),
            ],
        ),
        out_shape=(
            jax.ShapeDtypeStruct((4 * ROWS, d), bf16),
            jax.ShapeDtypeStruct((ROWS, d), f32),
        ),
        cost_estimate=cost(14),
        name="proj",
    )(at, core, *gated, gain, *rest)


def mixer_kernel(steps, outs, n_ref, w_ref, o1_ref, o2_ref, gu_v, dn_v, h_ref, sem):
    i = pl.program_id(0)
    units = steps * HD
    wide = o1_ref.shape[1]

    def gu_copy(t):
        src = w_ref.at[:, pl.ds(2 * HD * t, 2 * HD)]
        return pltpu.make_async_copy(src, gu_v.at[t], sem.at[t])

    def dn_copy(t):
        rows = pl.ds(wide * t, wide)
        src = w_ref.at[rows, pl.ds(2 * units, units)]
        return pltpu.make_async_copy(src, dn_v.at[rows, :], sem.at[steps + t])

    @pl.when(i == 0)
    def _():
        for t in range(steps):
            gu_copy(t).start()
        for t in range(outs):
            dn_copy(t).start()

    @pl.when(i < steps)
    def _():
        gu_copy(i).wait()
        both = dot(n_ref[...], gu_v[i])
        gate, up = both[:, :HD], both[:, HD:]
        h_ref[i] = (gate * jax.nn.sigmoid(gate) * up).astype(bf16)

    @pl.when(i >= steps)
    def _():
        t = i - steps
        dn_copy(t).wait()
        hidden = jnp.concatenate([h_ref[k] for k in range(steps)], axis=1)
        out = dot(hidden, dn_v[pl.ds(wide * t, wide), :], 1, 1).astype(bf16)
        o1_ref[...] = out[:ROWS]
        o2_ref[...] = out[ROWS:]


def mixer_call(normed, weights, block):
    d = normed.shape[1]
    units = weights.shape[1] // 3
    steps = units // HD
    wide = 512
    outs = d // wide
    rows = 2 * ROWS
    out = pl.BlockSpec((ROWS, wide), lambda i: (0, jnp.maximum(i - steps, 0)))
    return pl.pallas_call(
        functools.partial(mixer_kernel, steps, outs),
        grid=(steps + outs,),
        in_specs=[
            pl.BlockSpec((rows, d), lambda i: (block, 0)),
            pl.BlockSpec(memory_space=pl.ANY),
        ],
        out_specs=(out, out),
        out_shape=(jax.ShapeDtypeStruct((ROWS, d), bf16),) * 2,
        scratch_shapes=[
            pltpu.VMEM((steps, d, 2 * HD), bf16),
            pltpu.VMEM((d, units), bf16),
            pltpu.VMEM((steps, rows, HD), bf16),
            pltpu.SemaphoreType.DMA((steps + outs,)),
        ],
        cost_estimate=cost(16),
        name="mixer",
    )(normed, weights)


def shift(x, by, axis="tp", n=4):
    return lax.ppermute(x, axis, [(i, (i + by) % n) for i in range(n)])


def relative(x):
    return (x, shift(x, 1), shift(x, -1), shift(x, 2))


def body(
    query_rows,
    key_rows,
    value_rows,
    input_gate,
    forget_gate,
    output_gate,
    documents,
    residual,
    out_weight,
    norm_gain,
    gate_weight,
    up_weight,
    down_weight,
):
    me = lax.axis_index("tp")
    core = lax.axis_index("sp_2")
    docs = documents.reshape(1, TOK)
    k_rows, units = gate_weight.shape
    tiles = units // HD
    pair = jnp.concatenate(
        [gate_weight.reshape(k_rows, tiles, 1, HD), up_weight.reshape(k_rows, tiles, 1, HD)], axis=2
    ).reshape(k_rows, 2 * units)
    both = jnp.concatenate([pair, down_weight.T], axis=1)
    weights = lax.all_gather(both, SP, axis=0, tiled=True)
    half = lax.dynamic_slice_in_dim(out_weight, core * PART, PART, 0)
    packed = jnp.concatenate([residual[:PART], half, residual[PART:]], axis=0)
    left, right = shift(packed, 1), shift(packed, -1)
    state, a = state_call(key_rows, value_rows, input_gate, forget_gate, docs)
    above = lax.ppermute(state, "sp_0", [(0, 1), (1, 2), (2, 3)])
    row = lax.axis_index("sp_1")
    earlier = [shift(jnp.where(row + d < 4, state, above), d, "sp_1") for d in (1, 2, 3)]
    far = jnp.concatenate([state, *earlier], axis=0)
    near = shift(far, 1, "sp_2", 2)
    num, aux = local_call(query_rows, key_rows, value_rows, a, docs)
    left, right, num = lax.optimization_barrier((left, right, num))
    gated = join_call(core.reshape(1), far, near, query_rows, num, aux, output_gate)
    around = relative(gated)
    cut = packed.shape[0] // 2
    opp_a, opp_b = shift(left[:cut], 1), shift(right[cut:], -1)
    partner = [
        shift(part, 1, "sp_2", 2)
        for part in (
            left[PART : 2 * PART],
            right[PART : 2 * PART],
            opp_a[PART:],
            opp_b[: PART // 2],
        )
    ]
    offset = jnp.array([(0, 3, 1, 2)[g] for g, _ in BLOCKS], jnp.int32)
    part = jnp.array([h for _, h in BLOCKS], jnp.int32)
    at = (me + offset) % 4 * 2 + part
    normed, stream = proj_call(
        at,
        core.reshape(1),
        around,
        norm_gain.reshape(1, -1),
        (out_weight, residual, left, right, opp_a, opp_b, *partner),
    )
    a1, a2 = mixer_call(normed, weights, 0)
    from_left, from_right = shift(a1, 1), shift(a2, -1)
    b1, own = mixer_call(normed, weights, 1)
    add = lambda x, y: (x.astype(f32) + y.astype(f32)).astype(bf16)
    to_right, to_left = lax.optimization_barrier(
        (add(b1[:PART], from_left[:PART]), add(b1[PART:], from_right[:PART]))
    )
    late_left, late_right = shift(to_right, 1), shift(to_left, -1)
    sent0 = late_left.astype(f32) + from_right[PART:].astype(f32)
    sent1 = late_right.astype(f32) + from_left[PART:].astype(f32)
    down = own.astype(f32) + jnp.concatenate([sent0, sent1], axis=0)
    return (stream + 0.5 * down).astype(bf16)


def solution(mesh):
    torus = Mesh(mesh.devices.reshape(4, 4, 2, mesh.shape["tp"]), ("sp_0", "sp_1", "sp_2", "tp"))
    in_specs = (
        P(SP, "tp"),
        P(SP, "tp"),
        P(SP, "tp"),
        P("tp", SP),
        P("tp", SP),
        P(SP, "tp"),
        P(SP),
        P(SP_TP, None),
        P("tp", None),
        P(),
        P(SP, "tp"),
        P(SP, "tp"),
        P("tp", SP),
    )
    out_specs = P(SP_TP, None)
    return jax.shard_map(body, mesh=torus, in_specs=in_specs, out_specs=out_specs, check_vma=False)
```
